32 devices in a mesh: fs: 4 (over z), rep: 4 (over y, x), tp: 2 (over core).
Axes of the slice: x: 2, y: 2, z: 4, core: 2. Of those that a mesh axis runs over, the one named last changes fastest.
Arguments:
- inputs: bfloat16 [2048, 2048], P(('fs', 'rep')), may hold values from -6 to 6
- query_cot: bfloat16 [2048, 1024], P(('fs', 'rep'), 'tp'), may hold values from -0.125 to 0.125
- attended: bfloat16 [2048, 1024], P(('fs', 'rep')), may hold values from -6 to 6
- output_cot: bfloat16 [2048, 2048], P(('fs', 'rep'), 'tp'), may hold values from -0.125 to 0.125
- proj_query: bfloat16 [2048, 256], P('fs'), may hold values from -0.125 to 0.125
- proj_output: bfloat16 [1024, 256], P('fs'), may hold values from -0.1875 to 0.1875
- weight_query: float32 [2048, 1024], P('fs', 'tp'), may hold values from -0.125 to 0.125
- weight_output: float32 [1024, 2048], P('fs', 'tp'), may hold values from -0.1875 to 0.1875
- first_query: float32 [256, 1024], P('fs', 'tp'), may hold values from -6 to 6
- second_query: float32 [256, 1024], P('fs', 'tp'), may hold values from 0.0002 to 2
- first_output: float32 [256, 2048], P('fs', 'tp'), may hold values from -6 to 6
- second_output: float32 [256, 2048], P('fs', 'tp'), may hold values from 0.0002 to 2
Outputs:
- new_weight_query: float32 [2048, 1024], P('fs', 'tp')
- new_weight_output: float32 [1024, 2048], P('fs', 'tp')
- step_query: float32 [2048, 1024], P('fs', 'tp')
- step_output: float32 [1024, 2048], P('fs', 'tp')
- new_first_query: float32 [256, 1024], P('fs', 'tp')
- new_second_query: float32 [256, 1024], P('fs', 'tp')
- new_first_output: float32 [256, 2048], P('fs', 'tp')
- new_second_output: float32 [256, 2048], P('fs', 'tp')
- copy_query: bfloat16 [2048, 1024], P(None, 'tp')
- copy_output: bfloat16 [1024, 2048], P(None, 'tp')
The draws below stay inside these ranges and needn't reach their ends.
All inputs are finite; a program needn't handle non-finite values.
Results may differ from the reference program's by a relative error of at most 0.0031.
Values may be sent and summed in bfloat16 or wider, within the bound.
A program may use at most 64 MiB of HBM per device.

```python
import jax
import jax.numpy as jnp
from jax import lax

D = 2048
DA = 1024
RANK = 256
TOKENS = 2048


def variance_table(key, height, breadth):
    base = jnp.exp(jax.random.uniform(key, (height, breadth), jnp.float32, jnp.log(0.02), jnp.log(1.0)))
    row_place = jnp.arange(height, dtype=jnp.float32) / height
    col_place = jnp.arange(breadth, dtype=jnp.float32) / breadth
    return base * jnp.exp(-jnp.log(10.0) * row_place)[:, None] * jnp.exp(-jnp.log(10.0) * col_place)[None, :]


def draw_second_query(key, part):
    return variance_table(jax.random.fold_in(key, 11), RANK, DA)


def draw_second_output(key, part):
    return variance_table(jax.random.fold_in(key, 12), RANK, D)


def with_spikes(drawn, stream_key, source, target, parts, factor):
    owner, partner = [(jnp.arange(drawn.shape[axis_at]) // (drawn.shape[axis_at] // parts)).reshape([-1 if axis == axis_at else 1 for axis in range(drawn.ndim)]) for axis_at in (source, target)]
    chosen = jax.random.permutation(stream_key, parts)[partner]
    strong = (owner == chosen) | (owner == (partner + parts // 2) % parts)
    return jnp.where(strong, factor * drawn, drawn)


def block_scale(own_key, extent, cuts, least, top_value):
    factor_of = 1.0
    for axis_at, shards_of in cuts:
        draws = jax.random.uniform(jax.random.fold_in(jax.random.fold_in(own_key, 6), axis_at), (shards_of,), jnp.float32, least / len(cuts), top_value / len(cuts))
        factor_of = factor_of * jnp.repeat(jnp.exp(draws), extent[axis_at] // shards_of).reshape((-1,) + (1,) * (len(extent) - 1 - axis_at))
    return factor_of


def scatter_about(rng, extent, scale, most, pieces=(), kind=jnp.bfloat16):
    values = scale * jax.random.normal(rng, extent, jnp.float32)
    if pieces:
        values = values * block_scale(rng, extent, pieces, -0.22, 0.18)
    return jnp.clip(values, -most, most).astype(kind)


def bell_draw_with(key, shape, scale, reach, pieces, heavy, kind=jnp.bfloat16):
    values = scale * jax.random.normal(key, shape, jnp.float32)
    if pieces:
        values = values * block_scale(key, shape, pieces, -0.22, 0.18)
    return jnp.clip(with_spikes(values, jax.random.fold_in(key, 3), *heavy), -reach, reach).astype(kind)


def setup_inputs(seed: int = 0) -> dict:
    keys = jax.random.split(jax.random.key(seed), 13)
    inputs = bell_draw_with(keys[0], (TOKENS, D), 1.0, 6.0, ((0, 16),), (0, 1, 16, 2.0))
    query_cot = scatter_about(keys[1], (TOKENS, DA), TOKENS ** -0.5, 0.125, ((0, 16), (1, 2)))
    attended = bell_draw_with(keys[2], (TOKENS, DA), 1.0, 6.0, ((0, 16),), (0, 1, 16, 2.0))
    output_cot = scatter_about(keys[3], (TOKENS, D), TOKENS ** -0.5, 0.125, ((0, 16), (1, 2)))
    proj_query = scatter_about(keys[4], (D, RANK), D ** -0.5, 0.125, ((0, 4),))
    proj_output = scatter_about(keys[5], (DA, RANK), DA ** -0.5, 0.1875, ((0, 4),))
    weight_query = scatter_about(keys[6], (D, DA), D ** -0.5, 0.125, ((0, 4), (1, 2)), jnp.float32)
    weight_output = scatter_about(keys[7], (DA, D), DA ** -0.5, 0.1875, ((0, 4), (1, 2)), jnp.float32)
    first_query = scatter_about(keys[8], (RANK, DA), 1.0, 6.0, ((0, 4), (1, 2)), jnp.float32)
    second_query = draw_second_query(jax.random.fold_in(keys[12], 71), 0)
    first_output = scatter_about(keys[10], (RANK, D), 1.0, 6.0, ((0, 4), (1, 2)), jnp.float32)
    second_output = draw_second_output(jax.random.fold_in(keys[12], 71), 0)
    return dict(inputs=inputs, query_cot=query_cot, attended=attended, output_cot=output_cot, proj_query=proj_query, proj_output=proj_output, weight_query=weight_query, weight_output=weight_output, first_query=first_query, second_query=second_query, first_output=first_output, second_output=second_output)


beta_first = 0.9
beta_second = 0.95
adam_eps = 1e-08
mean_eps = 1e-06
learn_rate = 0.02

def contract_rows(left, right, high):
    if high:
        return lax.dot_general(left, right, (((0,), (0,)), ((), ())), precision=lax.Precision.HIGHEST, preferred_element_type=jnp.float32)
    return lax.dot_general(left, right, (((0,), (0,)), ((), ())), preferred_element_type=jnp.float32)

def moment_update(low_sum, first, second):
    first_new = beta_first * first + (1.0 - beta_first) * low_sum
    second_new = beta_second * second + (1.0 - beta_second) * low_sum * low_sum
    normed = first_new / (jnp.sqrt(second_new) + adam_eps)
    return (first_new, second_new, normed)

def reference(inputs, query_cot, attended, output_cot, proj_query, proj_output, weight_query, weight_output, first_query, second_query, first_output, second_output):
    grad_query = contract_rows(inputs, query_cot, False)
    grad_output = contract_rows(attended, output_cot, False)
    low_query = contract_rows(proj_query.astype(jnp.float32), grad_query, True)
    low_output = contract_rows(proj_output.astype(jnp.float32), grad_output, True)
    first_q, second_q, normed_q = moment_update(low_query, first_query, second_query)
    first_o, second_o, normed_o = moment_update(low_output, first_output, second_output)
    entries = RANK * (DA + D)
    total = jnp.sum(normed_q * normed_q) + jnp.sum(normed_o * normed_o)
    scale = lax.rsqrt(total / entries + mean_eps)
    half_q = normed_q.astype(jnp.bfloat16)
    half_o = normed_o.astype(jnp.bfloat16)
    step_q = scale * jnp.dot(proj_query, half_q, preferred_element_type=jnp.float32)
    step_o = scale * jnp.dot(proj_output, half_o, preferred_element_type=jnp.float32)
    new_q = weight_query - learn_rate * step_q
    new_o = weight_output - learn_rate * step_o
    return (new_q, new_o, step_q, step_o, first_q, second_q, first_o, second_o, new_q.astype(jnp.bfloat16), new_o.astype(jnp.bfloat16))
```

```python
import functools

import jax
import jax.numpy as jnp
from jax import lax
from jax.experimental import pallas as pl
from jax.experimental.pallas import tpu as pltpu
from jax.sharding import PartitionSpec as P

beta_first = 0.9
beta_second = 0.95
adam_eps = 1e-08
mean_eps = 1e-06
learn_rate = 0.02

MESH = pl.DeviceIdType.MESH
F32 = jnp.float32
BF16 = jnp.bfloat16


def kernel(
    n, r, tp, entries,
    x_ref, qc_ref, a_ref, oc_ref, pq_ref, po_ref, wq_ref, wo_ref, fq_ref, sq_ref, fo_ref, so_ref,
    nwq, nwo, stq, sto, nfq, nsq, nfo, nso, cpq, cpo,
    allq, allo, allx, alla, allqc, alloc, sbuf, r2, lowg, half, tz, tr, tt,
    pz_s, pz_r, pt_s, pt_r, xr_s, xr_r, xt_s, xt_r, cr1_s, cr1_r, r2_s, r2_r, lg_s, lg_r, hz_s, hz_r, hr_s, hr_r,
    tz_s, tz_r, tr_s, tr_r, tt_s, tt_r, cz_s, cz_r, cr_s, cr_r,
):
    f, k, t = lax.axis_index("fs"), lax.axis_index("rep"), lax.axis_index("tp")
    other = {"tp": 1 - t}
    rows_q, rank = pq_ref.shape
    rows_o = po_ref.shape[0]
    low_rows = fq_ref.shape[0]
    quarter_q, quarter_o = fq_ref.shape[1] // r, fo_ref.shape[1] // r
    fs_peers = [lax.rem(f + d, n) for d in range(1, n)]
    rep_peers = [lax.rem(k + d, r) for d in range(1, r)]

    def send(src, dst, ssem, rsem, where):
        copy = pltpu.make_async_remote_copy(
            src_ref=src, dst_ref=dst, send_sem=ssem, recv_sem=rsem, device_id=where, device_id_type=MESH
        )
        copy.start()
        return copy

    def arrived(dst, ssem, rsem, where):
        pltpu.make_async_remote_copy(
            src_ref=dst, dst_ref=dst, send_sem=ssem, recv_sem=rsem, device_id=where, device_id_type=MESH
        ).wait_recv()

    def cols(index, width):
        return pl.ds(pl.multiple_of(index * width, width), width)

    barrier = pltpu.get_barrier_semaphore()
    for j in fs_peers:
        pl.semaphore_signal(barrier, inc=1, device_id={"fs": j}, device_id_type=MESH)
    for j in rep_peers:
        pl.semaphore_signal(barrier, inc=1, device_id={"rep": j}, device_id_type=MESH)
    pl.semaphore_signal(barrier, inc=1, device_id=other, device_id_type=MESH)
    pl.semaphore_wait(barrier, n - 1 + r - 1 + 1)

    sent = []
    tokens = x_ref.shape[0]
    pieces = ((pq_ref, allq, rows_q // tp, 0), (po_ref, allo, rows_o // tp, 1))
    loads = ((x_ref, allx, tokens // tp, 0), (a_ref, alla, tokens // tp, 1))
    for j in fs_peers:
        for own, whole, part, i in pieces:
            mine = cols(t, part)
            sent.append(send(own.at[mine], whole.at[f, mine], pz_s.at[i, j], pz_r.at[i, f], {"fs": j}))
    for j in rep_peers:
        for own, whole, part, i in loads:
            mine = cols(t, part)
            sent.append(send(own.at[mine], whole.at[k, mine], xr_s.at[i, j], xr_r.at[i, k], {"rep": j}))
    for j in rep_peers:
        for own, whole, width, i in ((qc_ref, allqc, quarter_q, 0), (oc_ref, alloc, quarter_o, 1)):
            sent.append(send(own.at[:, cols(j, width)], whole.at[k], cr1_s.at[i, j], cr1_r.at[i, k], {"rep": j}))
    allq[f] = pq_ref[...]
    allo[f] = po_ref[...]
    allx[k] = x_ref[...]
    alla[k] = a_ref[...]
    allqc[k] = qc_ref[:, cols(k, quarter_q)]
    alloc[k] = oc_ref[:, cols(k, quarter_o)]
    for d in range(max(n, r) - 1):
        for peers, group, s1, r1, s2, r2_, axis in (
            (fs_peers, pieces, pz_s, pz_r, pt_s, pt_r, "fs"),
            (rep_peers, loads, xr_s, xr_r, xt_s, xt_r, "rep"),
        ):
            if d >= len(peers):
                continue
            j = peers[d]
            for own, whole, part, i in group:
                mine = cols(t, part)
                arrived(whole.at[j, mine], s1.at[i, j], r1.at[i, j], {axis: j})
                sent.append(send(whole.at[j, mine], whole.at[j, mine], s2.at[i, j], r2_.at[i, j], other))
    for peers, group, s2, r2_ in ((fs_peers, pieces, pt_s, pt_r), (rep_peers, loads, xt_s, xt_r)):
        for j in peers:
            for own, whole, part, i in group:
                arrived(whole.at[j, cols(1 - t, part)], s2.at[i, j], r2_.at[i, j], other)
    for j in rep_peers:
        for whole, i in ((allqc, 0), (alloc, 1)):
            arrived(whole.at[j], cr1_s.at[i, j], cr1_r.at[i, j], {"rep": j})

    def projected(load, factor, cot):
        load, factor, cot = (v[...].reshape(-1, v.shape[-1]) for v in (load, factor, cot))
        turned = jnp.dot(load, factor, preferred_element_type=F32).T
        high = turned.astype(BF16)
        rest = (turned - high.astype(F32)).astype(BF16)
        return jnp.dot(high, cot, preferred_element_type=F32) + jnp.dot(rest, cot, preferred_element_type=F32)

    total_q = projected(allx, allq, allqc)
    total_o = projected(alla, allo, alloc)
    sbuf[:, :, :quarter_q] = total_q.reshape(n, low_rows, quarter_q)
    sbuf[:, :, quarter_q:] = total_o.reshape(n, low_rows, quarter_o)
    for j in fs_peers:
        sent.append(send(sbuf.at[j], r2.at[f], r2_s.at[j], r2_r.at[f], {"fs": j}))
    low = sbuf[f]
    for j in fs_peers:
        arrived(r2.at[j], r2_s.at[j], r2_r.at[j], {"fs": j})
        low += r2[j]
    lowg[k] = low

    def update(low_sum, first, second):
        first_new = beta_first * first + (1.0 - beta_first) * low_sum
        second_new = beta_second * second + (1.0 - beta_second) * low_sum * low_sum
        return first_new, second_new, first_new / (jnp.sqrt(second_new) + adam_eps)

    at_q, at_o = cols(k, quarter_q), cols(k, quarter_o)
    normed_q = update(low[:, :quarter_q], fq_ref[:, at_q], sq_ref[:, at_q])[2]
    normed_o = update(low[:, quarter_q:], fo_ref[:, at_o], so_ref[:, at_o])[2]
    half[k, f, :, :quarter_q] = normed_q.astype(BF16)
    half[k, f, :, quarter_q:] = normed_o.astype(BF16)
    share = jnp.sum(normed_q * normed_q) + jnp.sum(normed_o * normed_o)
    tz[f] = jnp.full(tz.shape[1:], share, F32)
    for j in fs_peers:
        sent.append(send(tz.at[f], tz.at[f], tz_s.at[j], tz_r.at[f], {"fs": j}))
        sent.append(send(half.at[k, f], half.at[k, f], hz_s.at[j], hz_r.at[f], {"fs": j}))
    for j in rep_peers:
        sent.append(send(half.at[k, f], half.at[k, f], hr_s.at[f, j], hr_r.at[f, k], {"rep": j}))

    for j in fs_peers:
        arrived(tz.at[j], tz_s.at[j], tz_r.at[j], {"fs": j})
    tr[k] = jnp.sum(tz[...], axis=0)
    for j in rep_peers:
        sent.append(send(tr.at[k], tr.at[k], tr_s.at[j], tr_r.at[k], {"rep": j}))
    for j in fs_peers:
        arrived(half.at[k, j], hz_s.at[j], hz_r.at[j], {"fs": j})
        for m in rep_peers:
            sent.append(send(half.at[k, j], half.at[k, j], hr_s.at[j, m], hr_r.at[j, k], {"rep": m}))
    for j in rep_peers:
        arrived(tr.at[j], tr_s.at[j], tr_r.at[j], {"rep": j})
    tt[t] = jnp.sum(tr[...], axis=0)
    sent.append(send(tt.at[t], tt.at[t], tt_s.at[0], tt_r.at[0], other))

    def weights(index, scale):
        block = half[index].reshape(rank, quarter_q + quarter_o)
        for proj, lo, hi, width, old, new, step, copy, rows in (
            (pq_ref, 0, quarter_q, quarter_q, wq_ref, nwq, stq, cpq, rows_q),
            (po_ref, quarter_q, quarter_q + quarter_o, quarter_o, wo_ref, nwo, sto, cpo, rows_o),
        ):
            at = cols(index, width)
            moved = scale * jnp.dot(proj[...], block[:, lo:hi], preferred_element_type=F32)
            fresh = old[:, at] - learn_rate * moved
            step[:, at] = moved
            new[:, at] = fresh
            copy[cols(f, rows), at] = fresh.astype(BF16)

    arrived(tt.at[1 - t], tt_s.at[0], tt_r.at[0], other)
    scale = lax.rsqrt((tt[0] + tt[1])[:1, :1] / entries + mean_eps)
    weights(k, scale)
    outs = ((cpq, rows_q, quarter_q, 0), (cpo, rows_o, quarter_o, 1))
    for j in fs_peers:
        for copy, rows, width, i in outs:
            block = copy.at[cols(f, rows), cols(k, width)]
            sent.append(send(block, block, cz_s.at[i, j], cz_r.at[i, f], {"fs": j}))
    for j in rep_peers:
        sent.append(send(lowg.at[k], lowg.at[k], lg_s.at[j], lg_r.at[k], {"rep": j}))
    for m in rep_peers:
        for j in [f] + fs_peers:
            arrived(half.at[m, j], hr_s.at[j, m], hr_r.at[j, m], {"rep": m})
        weights(m, scale)
    for j in fs_peers:
        for copy, rows, width, i in outs:
            block = copy.at[cols(j, rows), cols(k, width)]
            arrived(block, cz_s.at[i, j], cz_r.at[i, j], {"fs": j})
            for m in rep_peers:
                sent.append(send(block, block, cr_s.at[i, j, m], cr_r.at[i, j, k], {"rep": m}))
    for m in [k] + rep_peers:
        if m is not k:
            arrived(lowg.at[m], lg_s.at[m], lg_r.at[m], {"rep": m})
        block = lowg[m]
        at_q, at_o = cols(m, quarter_q), cols(m, quarter_o)
        nfq[:, at_q], nsq[:, at_q], _ = update(block[:, :quarter_q], fq_ref[:, at_q], sq_ref[:, at_q])
        nfo[:, at_o], nso[:, at_o], _ = update(block[:, quarter_q:], fo_ref[:, at_o], so_ref[:, at_o])
    for j in fs_peers:
        for m in rep_peers:
            for copy, rows, width, i in outs:
                block = copy.at[cols(j, rows), cols(m, width)]
                arrived(block, cr_s.at[i, j, m], cr_r.at[i, j, m], {"rep": m})
    for copy in sent:
        copy.wait_send()


def solution(mesh):
    n, r, tp = mesh.shape["fs"], mesh.shape["rep"], mesh.shape["tp"]

    def local(*args):
        x, qc, a, oc, pq, po, wq, wo, fq, sq, fo, so = args
        rank = pq.shape[1]
        low_rows = fq.shape[0]
        wide = (fq.shape[1] + fo.shape[1]) // r
        entries = rank * (fq.shape[1] + fo.shape[1]) * tp
        shape = jax.ShapeDtypeStruct
        like = lambda v: shape(v.shape, v.dtype)
        dma = pltpu.SemaphoreType.DMA
        return pl.pallas_call(
            functools.partial(kernel, n, r, tp, entries),
            out_shape=(
                like(wq), like(wo), like(wq), like(wo), like(fq), like(sq), like(fo), like(so),
                shape((n * wq.shape[0], wq.shape[1]), BF16),
                shape((n * wo.shape[0], wo.shape[1]), BF16),
            ),
            in_specs=[pl.BlockSpec(memory_space=pltpu.VMEM)] * 12,
            out_specs=[pl.BlockSpec(memory_space=pltpu.VMEM)] * 10,
            scratch_shapes=[
                pltpu.VMEM((n,) + pq.shape, BF16),
                pltpu.VMEM((n,) + po.shape, BF16),
                pltpu.VMEM((r,) + x.shape, BF16),
                pltpu.VMEM((r,) + a.shape, BF16),
                pltpu.VMEM((r, qc.shape[0], qc.shape[1] // r), BF16),
                pltpu.VMEM((r, oc.shape[0], oc.shape[1] // r), BF16),
                pltpu.VMEM((n, low_rows, wide), F32),
                pltpu.VMEM((n, low_rows, wide), F32),
                pltpu.VMEM((r, low_rows, wide), F32),
                pltpu.VMEM((r, n, low_rows, wide), BF16),
                pltpu.VMEM((n, 8, 128), F32),
                pltpu.VMEM((r, 8, 128), F32),
                pltpu.VMEM((tp, 8, 128), F32),
                dma((2, n)), dma((2, n)), dma((2, n)), dma((2, n)),
                dma((2, r)), dma((2, r)), dma((2, r)), dma((2, r)), dma((2, r)), dma((2, r)), dma((n,)), dma((n,)), dma((r,)), dma((r,)),
                dma((n,)), dma((n,)), dma((n, r)), dma((n, r)),
                dma((n,)), dma((n,)), dma((r,)), dma((r,)), dma((1,)), dma((1,)),
                dma((2, n)), dma((2, n)), dma((2, n, r)), dma((2, n, r)),
            ],
            compiler_params=pltpu.CompilerParams(collective_id=0, has_side_effects=True),
        )(*args)

    both, rows = P(("fs", "rep"), "tp"), P("fs", "tp")
    whole = P(("fs", "rep"), None)
    return jax.shard_map(
        local,
        mesh=mesh,
        in_specs=(whole, both, whole, both, P("fs", None), P("fs", None)) + (rows,) * 6,
        out_specs=(rows,) * 8 + (P(None, "tp"),) * 2,
        check_vma=False,
    )
```

```python
import functools

import jax
import jax.numpy as jnp
from jax import lax
from jax.experimental import pallas as pl
from jax.experimental.pallas import tpu as pltpu
from jax.sharding import PartitionSpec as P

beta_first = 0.9
beta_second = 0.95
adam_eps = 1e-08
mean_eps = 1e-06
learn_rate = 0.02

MESH = pl.DeviceIdType.MESH
F32 = jnp.float32
BF16 = jnp.bfloat16


def kernel(
    n, r, tp, entries,
    x_ref, qc_ref, a_ref, oc_ref, pq_ref, po_ref, wq_ref, wo_ref, fq_ref, sq_ref, fo_ref, so_ref,
    nwq, nwo, stq, sto, nfq, nsq, nfo, nso, cpq, cpo,
    allq, allo, allx, alla, allqc, alloc, sbuf, r2, lowg, half, tz, tr, tt,
    pz_s, pz_r, pt_s, pt_r, xr_s, xr_r, xt_s, xt_r, cr1_s, cr1_r, r2_s, r2_r, lg_s, lg_r, hz_s, hz_r, hr_s, hr_r,
    tz_s, tz_r, tr_s, tr_r, tt_s, tt_r, cz_s, cz_r, cr_s, cr_r,
):
    f, k, t = lax.axis_index("fs"), lax.axis_index("rep"), lax.axis_index("tp")
    other = {"tp": 1 - t}
    rows_q, rank = pq_ref.shape
    rows_o = po_ref.shape[0]
    low_rows = fq_ref.shape[0]
    quarter_q, quarter_o = fq_ref.shape[1] // r, fo_ref.shape[1] // r
    fs_peers = [lax.rem(f + d, n) for d in range(1, n)]
    rep_peers = [lax.rem(k + d, r) for d in range(1, r)]
    from_fs, from_rep = fs_peers[::-1], rep_peers[::-1]

    def send(src, dst, ssem, rsem, where):
        copy = pltpu.make_async_remote_copy(
            src_ref=src, dst_ref=dst, send_sem=ssem, recv_sem=rsem, device_id=where, device_id_type=MESH
        )
        copy.start()
        return copy

    def arrived(dst, ssem, rsem, where):
        pltpu.make_async_remote_copy(
            src_ref=dst, dst_ref=dst, send_sem=ssem, recv_sem=rsem, device_id=where, device_id_type=MESH
        ).wait_recv()

    def cols(index, width):
        return pl.ds(pl.multiple_of(index * width, width), width)

    barrier = pltpu.get_barrier_semaphore()
    for j in fs_peers:
        pl.semaphore_signal(barrier, inc=1, device_id={"fs": j}, device_id_type=MESH)
    for j in rep_peers:
        pl.semaphore_signal(barrier, inc=1, device_id={"rep": j}, device_id_type=MESH)
    pl.semaphore_signal(barrier, inc=1, device_id=other, device_id_type=MESH)
    pl.semaphore_wait(barrier, n - 1 + r - 1 + 1)

    sent = []
    tokens = x_ref.shape[0]
    pieces = ((pq_ref, allq, rows_q // tp, 0), (po_ref, allo, rows_o // tp, 1))
    loads = ((x_ref, allx, tokens // tp, 0), (a_ref, alla, tokens // tp, 1))
    for j in fs_peers:
        for own, whole, part, i in pieces:
            mine = cols(t, part)
            sent.append(send(own.at[mine], whole.at[f, mine], pz_s.at[i, j], pz_r.at[i, f], {"fs": j}))
    for j in rep_peers:
        for own, whole, part, i in loads:
            mine = cols(t, part)
            sent.append(send(own.at[mine], whole.at[k, mine], xr_s.at[i, j], xr_r.at[i, k], {"rep": j}))
    for j in rep_peers:
        for own, whole, width, i in ((qc_ref, allqc, quarter_q, 0), (oc_ref, alloc, quarter_o, 1)):
            sent.append(send(own.at[:, cols(j, width)], whole.at[k], cr1_s.at[i, j], cr1_r.at[i, k], {"rep": j}))
    allq[f] = pq_ref[...]
    allo[f] = po_ref[...]
    allx[k] = x_ref[...]
    alla[k] = a_ref[...]
    allqc[k] = qc_ref[:, cols(k, quarter_q)]
    alloc[k] = oc_ref[:, cols(k, quarter_o)]
    for d in range(max(n, r) - 1):
        for peers, group, s1, r1, s2, r2_, axis in (
            (from_fs, pieces, pz_s, pz_r, pt_s, pt_r, "fs"),
            (from_rep, loads, xr_s, xr_r, xt_s, xt_r, "rep"),
        ):
            if d >= len(peers):
                continue
            j = peers[d]
            for own, whole, part, i in group:
                mine = cols(t, part)
                arrived(whole.at[j, mine], s1.at[i, j], r1.at[i, j], {axis: j})
                sent.append(send(whole.at[j, mine], whole.at[j, mine], s2.at[i, j], r2_.at[i, j], other))
    for peers, group, s2, r2_ in ((fs_peers, pieces, pt_s, pt_r), (rep_peers, loads, xt_s, xt_r)):
        for j in peers:
            for own, whole, part, i in group:
                arrived(whole.at[j, cols(1 - t, part)], s2.at[i, j], r2_.at[i, j], other)
    for j in rep_peers:
        for whole, i in ((allqc, 0), (alloc, 1)):
            arrived(whole.at[j], cr1_s.at[i, j], cr1_r.at[i, j], {"rep": j})

    def projected(load, factor, cot):
        load, factor, cot = (v[...].reshape(-1, v.shape[-1]) for v in (load, factor, cot))
        turned = jnp.dot(load, factor, preferred_element_type=F32).T
        high = turned.astype(BF16)
        rest = (turned - high.astype(F32)).astype(BF16)
        return jnp.dot(high, cot, preferred_element_type=F32) + jnp.dot(rest, cot, preferred_element_type=F32)

    total_q = projected(allx, allq, allqc)
    total_o = projected(alla, allo, alloc)
    sbuf[:, :, :quarter_q] = total_q.reshape(n, low_rows, quarter_q)
    sbuf[:, :, quarter_q:] = total_o.reshape(n, low_rows, quarter_o)
    for j in fs_peers:
        sent.append(send(sbuf.at[j], r2.at[f], r2_s.at[j], r2_r.at[f], {"fs": j}))
    low = sbuf[f]
    for j in fs_peers:
        arrived(r2.at[j], r2_s.at[j], r2_r.at[j], {"fs": j})
        low += r2[j]
    lowg[k] = low

    def update(low_sum, first, second):
        first_new = beta_first * first + (1.0 - beta_first) * low_sum
        second_new = beta_second * second + (1.0 - beta_second) * low_sum * low_sum
        return first_new, second_new, first_new / (jnp.sqrt(second_new) + adam_eps)

    at_q, at_o = cols(k, quarter_q), cols(k, quarter_o)
    normed_q = update(low[:, :quarter_q], fq_ref[:, at_q], sq_ref[:, at_q])[2]
    normed_o = update(low[:, quarter_q:], fo_ref[:, at_o], so_ref[:, at_o])[2]
    half[k, f, :, :quarter_q] = normed_q.astype(BF16)
    half[k, f, :, quarter_q:] = normed_o.astype(BF16)
    share = jnp.sum(normed_q * normed_q) + jnp.sum(normed_o * normed_o)
    tz[f] = jnp.full(tz.shape[1:], share, F32)
    for j in fs_peers:
        sent.append(send(tz.at[f], tz.at[f], tz_s.at[j], tz_r.at[f], {"fs": j}))
        sent.append(send(half.at[k, f], half.at[k, f], hz_s.at[j], hz_r.at[f], {"fs": j}))
    for j in rep_peers:
        sent.append(send(half.at[k, f], half.at[k, f], hr_s.at[f, j], hr_r.at[f, k], {"rep": j}))

    for j in fs_peers:
        arrived(tz.at[j], tz_s.at[j], tz_r.at[j], {"fs": j})
    tr[k] = jnp.sum(tz[...], axis=0)
    for j in rep_peers:
        sent.append(send(tr.at[k], tr.at[k], tr_s.at[j], tr_r.at[k], {"rep": j}))
    for j in from_fs:
        arrived(half.at[k, j], hz_s.at[j], hz_r.at[j], {"fs": j})
        for m in rep_peers:
            sent.append(send(half.at[k, j], half.at[k, j], hr_s.at[j, m], hr_r.at[j, k], {"rep": m}))
    for j in rep_peers:
        arrived(tr.at[j], tr_s.at[j], tr_r.at[j], {"rep": j})
    tt[t] = jnp.sum(tr[...], axis=0)
    sent.append(send(tt.at[t], tt.at[t], tt_s.at[0], tt_r.at[0], other))

    def weights(index, scale):
        block = half[index].reshape(rank, quarter_q + quarter_o)
        for proj, lo, hi, width, old, new, step, copy, rows in (
            (pq_ref, 0, quarter_q, quarter_q, wq_ref, nwq, stq, cpq, rows_q),
            (po_ref, quarter_q, quarter_q + quarter_o, quarter_o, wo_ref, nwo, sto, cpo, rows_o),
        ):
            at = cols(index, width)
            moved = scale * jnp.dot(proj[...], block[:, lo:hi], preferred_element_type=F32)
            fresh = old[:, at] - learn_rate * moved
            step[:, at] = moved
            new[:, at] = fresh
            copy[cols(f, rows), at] = fresh.astype(BF16)

    arrived(tt.at[1 - t], tt_s.at[0], tt_r.at[0], other)
    scale = lax.rsqrt((tt[0] + tt[1])[:1, :1] / entries + mean_eps)
    weights(k, scale)
    outs = ((cpq, rows_q, quarter_q, 0), (cpo, rows_o, quarter_o, 1))
    for j in fs_peers:
        for copy, rows, width, i in outs:
            block = copy.at[cols(f, rows), cols(k, width)]
            sent.append(send(block, block, cz_s.at[i, j], cz_r.at[i, f], {"fs": j}))
    for j in rep_peers:
        sent.append(send(lowg.at[k], lowg.at[k], lg_s.at[j], lg_r.at[k], {"rep": j}))
    for m in from_rep:
        for j in [f] + from_fs:
            arrived(half.at[m, j], hr_s.at[j, m], hr_r.at[j, m], {"rep": m})
        weights(m, scale)
    across = r == 4
    if across:
        near, far = k + 1 - 2 * lax.rem(k, 2), lax.rem(k + 2, r)
        beyond = lax.rem(near + 2, r)
        targets = [near, far]
    else:
        targets = rep_peers

    def block_of(i, j, m):
        copy, rows, width, _ = outs[i]
        return copy.at[cols(j, rows), cols(m, width)]

    def relay(j):
        for i, source, to in ((0, near, far), (1, far, near)):
            block = block_of(i, j, source)
            arrived(block, cr_s.at[i, j, source], cr_r.at[i, j, source], {"rep": source})
            sent.append(send(block, block, cr_s.at[i, j, beyond], cr_r.at[i, j, source], {"rep": to}))

    for step, j in enumerate(from_fs):
        for i in range(2):
            block = block_of(i, j, k)
            arrived(block, cz_s.at[i, j], cz_r.at[i, j], {"fs": j})
            for m in targets:
                sent.append(send(block, block, cr_s.at[i, j, m], cr_r.at[i, j, k], {"rep": m}))
        if across and step:
            relay(from_fs[step - 1])
    if across and from_fs:
        relay(from_fs[-1])
    for m in [k] + rep_peers:
        if m is not k:
            arrived(lowg.at[m], lg_s.at[m], lg_r.at[m], {"rep": m})
        block = lowg[m]
        at_q, at_o = cols(m, quarter_q), cols(m, quarter_o)
        nfq[:, at_q], nsq[:, at_q], _ = update(block[:, :quarter_q], fq_ref[:, at_q], sq_ref[:, at_q])
        nfo[:, at_o], nso[:, at_o], _ = update(block[:, quarter_q:], fo_ref[:, at_o], so_ref[:, at_o])
    late = ((1, near), (0, far), (0, beyond), (1, beyond)) if across else [(i, m) for m in from_rep for i in range(2)]
    for j in from_fs:
        for i, m in late:
            arrived(block_of(i, j, m), cr_s.at[i, j, m], cr_r.at[i, j, m], {"rep": m})
    for copy in sent:
        copy.wait_send()


def place(*refs):
    count = len(refs) // 2
    sems = refs[-1]
    copies = [pltpu.make_async_copy(refs[i], refs[count + i], sems.at[i]) for i in range(count)]
    for copy in copies:
        copy.start()
    for copy in copies:
        copy.wait()


def solution(mesh):
    n, r, tp = mesh.shape["fs"], mesh.shape["rep"], mesh.shape["tp"]

    def local(*args):
        x, qc, a, oc, pq, po, wq, wo, fq, sq, fo, so = args
        rank = pq.shape[1]
        low_rows = fq.shape[0]
        wide = (fq.shape[1] + fo.shape[1]) // r
        entries = rank * (fq.shape[1] + fo.shape[1]) * tp
        shape = jax.ShapeDtypeStruct
        like = lambda v: shape(v.shape, v.dtype)
        dma = pltpu.SemaphoreType.DMA
        made = pl.pallas_call(
            functools.partial(kernel, n, r, tp, entries),
            out_shape=(
                like(wq), like(wo), like(wq), like(wo), like(fq), like(sq), like(fo), like(so),
                shape((n * wq.shape[0], wq.shape[1]), BF16),
                shape((n * wo.shape[0], wo.shape[1]), BF16),
            ),
            in_specs=[pl.BlockSpec(memory_space=pltpu.VMEM)] * 12,
            out_specs=[pl.BlockSpec(memory_space=pltpu.VMEM)] * 10,
            scratch_shapes=[
                pltpu.VMEM((n,) + pq.shape, BF16),
                pltpu.VMEM((n,) + po.shape, BF16),
                pltpu.VMEM((r,) + x.shape, BF16),
                pltpu.VMEM((r,) + a.shape, BF16),
                pltpu.VMEM((r, qc.shape[0], qc.shape[1] // r), BF16),
                pltpu.VMEM((r, oc.shape[0], oc.shape[1] // r), BF16),
                pltpu.VMEM((n, low_rows, wide), F32),
                pltpu.VMEM((n, low_rows, wide), F32),
                pltpu.VMEM((r, low_rows, wide), F32),
                pltpu.VMEM((r, n, low_rows, wide), BF16),
                pltpu.VMEM((n, 8, 128), F32),
                pltpu.VMEM((r, 8, 128), F32),
                pltpu.VMEM((tp, 8, 128), F32),
                dma((2, n)), dma((2, n)), dma((2, n)), dma((2, n)),
                dma((2, r)), dma((2, r)), dma((2, r)), dma((2, r)), dma((2, r)), dma((2, r)), dma((n,)), dma((n,)), dma((r,)), dma((r,)),
                dma((n,)), dma((n,)), dma((n, r)), dma((n, r)),
                dma((n,)), dma((n,)), dma((r,)), dma((r,)), dma((1,)), dma((1,)),
                dma((2, n)), dma((2, n)), dma((2, n, r)), dma((2, n, r)),
            ],
            compiler_params=pltpu.CompilerParams(collective_id=0, has_side_effects=True),
        )(*args)
        return pl.pallas_call(
            place,
            out_shape=tuple(like(v) for v in made),
            in_specs=[pl.BlockSpec(memory_space=pltpu.VMEM)] * len(made),
            out_specs=[pl.BlockSpec(memory_space=pl.ANY)] * len(made),
            scratch_shapes=[dma((len(made),))],
        )(*made)

    both, rows = P(("fs", "rep"), "tp"), P("fs", "tp")
    whole = P(("fs", "rep"), None)
    return jax.shard_map(
        local,
        mesh=mesh,
        in_specs=(whole, both, whole, both, P("fs", None), P("fs", None)) + (rows,) * 6,
        out_specs=(rows,) * 8 + (P(None, "tp"),) * 2,
        check_vma=False,
    )
```

```python
import functools

import jax
import jax.numpy as jnp
from jax import lax
from jax.experimental import pallas as pl
from jax.experimental.pallas import tpu as pltpu
from jax.sharding import PartitionSpec as P

beta_first = 0.9
beta_second = 0.95
adam_eps = 1e-08
mean_eps = 1e-06
learn_rate = 0.02

MESH = pl.DeviceIdType.MESH
F32 = jnp.float32
BF16 = jnp.bfloat16


def kernel(
    n, r, tp, entries,
    x_ref, qc_ref, a_ref, oc_ref, pq_ref, po_ref, wq_ref, wo_ref, fq_ref, sq_ref, fo_ref, so_ref,
    nwq, nwo, stq, sto, nfq, nsq, nfo, nso, cpq, cpo,
    allq, allo, allx, alla, allqc, alloc, sbuf, r2, lowg, half, tz, tr, tt,
    pz_s, pz_r, pt_s, pt_r, xr_s, xr_r, xt_s, xt_r, cr1_s, cr1_r, r2_s, r2_r, lg_s, lg_r, hz_s, hz_r, hr_s, hr_r,
    tz_s, tz_r, tr_s, tr_r, tt_s, tt_r, cz_s, cz_r, cr_s, cr_r,
):
    f, k, t = lax.axis_index("fs"), lax.axis_index("rep"), lax.axis_index("tp")
    other = {"tp": 1 - t}
    rows_q, rank = pq_ref.shape
    rows_o = po_ref.shape[0]
    low_rows = fq_ref.shape[0]
    quarter_q, quarter_o = fq_ref.shape[1] // r, fo_ref.shape[1] // r
    fs_peers = [lax.rem(f + d, n) for d in range(1, n)]
    rep_peers = [lax.rem(k + d, r) for d in range(1, r)]
    from_fs, from_rep = fs_peers[::-1], rep_peers[::-1]
    across = r == 4
    if across:
        near, far = k + 1 - 2 * lax.rem(k, 2), lax.rem(k + 2, r)
        beyond = lax.rem(near + 2, r)
        targets = [near, far]
    else:
        targets = rep_peers

    def send(src, dst, ssem, rsem, where):
        copy = pltpu.make_async_remote_copy(
            src_ref=src, dst_ref=dst, send_sem=ssem, recv_sem=rsem, device_id=where, device_id_type=MESH
        )
        copy.start()
        return copy

    def arrived(dst, ssem, rsem, where):
        pltpu.make_async_remote_copy(
            src_ref=dst, dst_ref=dst, send_sem=ssem, recv_sem=rsem, device_id=where, device_id_type=MESH
        ).wait_recv()

    def cols(index, width):
        return pl.ds(pl.multiple_of(index * width, width), width)

    barrier = pltpu.get_barrier_semaphore()
    for j in fs_peers:
        pl.semaphore_signal(barrier, inc=1, device_id={"fs": j}, device_id_type=MESH)
    for j in rep_peers:
        pl.semaphore_signal(barrier, inc=1, device_id={"rep": j}, device_id_type=MESH)
    pl.semaphore_signal(barrier, inc=1, device_id=other, device_id_type=MESH)
    pl.semaphore_wait(barrier, n - 1 + r - 1 + 1)

    sent = []
    tokens = x_ref.shape[0]
    pieces = ((pq_ref, allq, rows_q // tp, 0), (po_ref, allo, rows_o // tp, 1))
    loads = ((x_ref, allx, tokens // tp, 0), (a_ref, alla, tokens // tp, 1))
    for j in fs_peers:
        for own, whole, part, i in pieces:
            mine = cols(t, part)
            sent.append(send(own.at[mine], whole.at[f, mine], pz_s.at[i, j], pz_r.at[i, f], {"fs": j}))
    for j in targets:
        for own, whole, part, i in loads:
            mine = cols(t, part)
            sent.append(send(own.at[mine], whole.at[k, mine], xr_s.at[i, j], xr_r.at[i, k], {"rep": j}))
    for j in rep_peers:
        for own, whole, width, i in ((qc_ref, allqc, quarter_q, 0), (oc_ref, alloc, quarter_o, 1)):
            sent.append(send(own.at[:, cols(j, width)], whole.at[k], cr1_s.at[i, j], cr1_r.at[i, k], {"rep": j}))
    allq[f] = pq_ref[...]
    allo[f] = po_ref[...]
    allx[k] = x_ref[...]
    alla[k] = a_ref[...]
    allqc[k] = qc_ref[:, cols(k, quarter_q)]
    alloc[k] = oc_ref[:, cols(k, quarter_o)]
    def hand_over(group, j, s1, r1, s2, r2_, axis):
        for own, whole, part, i in group:
            mine = cols(t, part)
            arrived(whole.at[j, mine], s1.at[i, j], r1.at[i, j], {axis: j})
            sent.append(send(whole.at[j, mine], whole.at[j, mine], s2.at[i, j], r2_.at[i, j], other))

    def half_rows(part, which):
        return cols(2 * t + which, part // 2)

    def pass_on(source, to, which):
        for own, whole, part, i in loads:
            rows = half_rows(part, which)
            block = whole.at[source, rows]
            sent.append(send(block, block, xr_s.at[i + 2 * which, beyond], xr_r.at[i + 2 * which, source], {"rep": to}))

    if across:
        for which, (source, to) in enumerate(((near, far), (far, near))):
            hand_over(loads, source, xr_s, xr_r, xt_s, xt_r, "rep")
            pass_on(source, to, which)
    else:
        for j in from_rep:
            hand_over(loads, j, xr_s, xr_r, xt_s, xt_r, "rep")
    for j in from_fs:
        hand_over(pieces, j, pz_s, pz_r, pt_s, pt_r, "fs")
    if across:
        for own, whole, part, i in loads:
            for which in range(2):
                block = whole.at[beyond, half_rows(part, which)]
                at = i + 2 * which
                arrived(block, xr_s.at[at, beyond], xr_r.at[at, beyond], {"rep": beyond})
                sent.append(send(block, block, xt_s.at[at, beyond], xt_r.at[at, beyond], other))
    for peers, group, s2, r2_ in ((fs_peers, pieces, pt_s, pt_r), (targets, loads, xt_s, xt_r)):
        for j in peers:
            for own, whole, part, i in group:
                arrived(whole.at[j, cols(1 - t, part)], s2.at[i, j], r2_.at[i, j], other)
    if across:
        for own, whole, part, i in loads:
            for which in range(2):
                block = whole.at[beyond, cols(2 * (1 - t) + which, part // 2)]
                at = i + 2 * which
                arrived(block, xt_s.at[at, beyond], xt_r.at[at, beyond], other)
    for j in rep_peers:
        for whole, i in ((allqc, 0), (alloc, 1)):
            arrived(whole.at[j], cr1_s.at[i, j], cr1_r.at[i, j], {"rep": j})

    def projected(load, factor, cot):
        load, factor, cot = (v[...].reshape(-1, v.shape[-1]) for v in (load, factor, cot))
        turned = jnp.dot(load, factor, preferred_element_type=F32).T
        high = turned.astype(BF16)
        rest = (turned - high.astype(F32)).astype(BF16)
        return jnp.dot(high, cot, preferred_element_type=F32) + jnp.dot(rest, cot, preferred_element_type=F32)

    total_q = projected(allx, allq, allqc)
    total_o = projected(alla, allo, alloc)
    sbuf[:, :, :quarter_q] = total_q.reshape(n, low_rows, quarter_q)
    sbuf[:, :, quarter_q:] = total_o.reshape(n, low_rows, quarter_o)
    for j in fs_peers:
        sent.append(send(sbuf.at[j], r2.at[f], r2_s.at[j], r2_r.at[f], {"fs": j}))
    low = sbuf[f]
    for j in fs_peers:
        arrived(r2.at[j], r2_s.at[j], r2_r.at[j], {"fs": j})
        low += r2[j]
    lowg[k] = low

    def update(low_sum, first, second):
        first_new = beta_first * first + (1.0 - beta_first) * low_sum
        second_new = beta_second * second + (1.0 - beta_second) * low_sum * low_sum
        return first_new, second_new, first_new / (jnp.sqrt(second_new) + adam_eps)

    at_q, at_o = cols(k, quarter_q), cols(k, quarter_o)
    normed_q = update(low[:, :quarter_q], fq_ref[:, at_q], sq_ref[:, at_q])[2]
    normed_o = update(low[:, quarter_q:], fo_ref[:, at_o], so_ref[:, at_o])[2]
    half[k, f, :, :quarter_q] = normed_q.astype(BF16)
    half[k, f, :, quarter_q:] = normed_o.astype(BF16)
    share = jnp.sum(normed_q * normed_q) + jnp.sum(normed_o * normed_o)
    tz[f] = jnp.full(tz.shape[1:], share, F32)
    for j in fs_peers:
        sent.append(send(tz.at[f], tz.at[f], tz_s.at[j], tz_r.at[f], {"fs": j}))
        sent.append(send(half.at[k, f], half.at[k, f], hz_s.at[j], hz_r.at[f], {"fs": j}))
    for j in rep_peers:
        sent.append(send(half.at[k, f], half.at[k, f], hr_s.at[f, j], hr_r.at[f, k], {"rep": j}))

    for j in fs_peers:
        arrived(tz.at[j], tz_s.at[j], tz_r.at[j], {"fs": j})
    tr[k] = jnp.sum(tz[...], axis=0)
    for j in rep_peers:
        sent.append(send(tr.at[k], tr.at[k], tr_s.at[j], tr_r.at[k], {"rep": j}))
    for j in from_fs:
        arrived(half.at[k, j], hz_s.at[j], hz_r.at[j], {"fs": j})
        for m in rep_peers:
            sent.append(send(half.at[k, j], half.at[k, j], hr_s.at[j, m], hr_r.at[j, k], {"rep": m}))
    for j in rep_peers:
        arrived(tr.at[j], tr_s.at[j], tr_r.at[j], {"rep": j})
    tt[t] = jnp.sum(tr[...], axis=0)
    sent.append(send(tt.at[t], tt.at[t], tt_s.at[0], tt_r.at[0], other))

    def weights(index, scale):
        block = half[index].reshape(rank, quarter_q + quarter_o)
        for proj, lo, hi, width, old, new, step, copy, rows in (
            (pq_ref, 0, quarter_q, quarter_q, wq_ref, nwq, stq, cpq, rows_q),
            (po_ref, quarter_q, quarter_q + quarter_o, quarter_o, wo_ref, nwo, sto, cpo, rows_o),
        ):
            at = cols(index, width)
            moved = scale * jnp.dot(proj[...], block[:, lo:hi], preferred_element_type=F32)
            fresh = old[:, at] - learn_rate * moved
            step[:, at] = moved
            new[:, at] = fresh
            copy[cols(f, rows), at] = fresh.astype(BF16)

    arrived(tt.at[1 - t], tt_s.at[0], tt_r.at[0], other)
    scale = lax.rsqrt((tt[0] + tt[1])[:1, :1] / entries + mean_eps)
    weights(k, scale)
    outs = ((cpq, rows_q, quarter_q, 0), (cpo, rows_o, quarter_o, 1))
    for j in fs_peers:
        for copy, rows, width, i in outs:
            block = copy.at[cols(f, rows), cols(k, width)]
            sent.append(send(block, block, cz_s.at[i, j], cz_r.at[i, f], {"fs": j}))
    for j in rep_peers:
        sent.append(send(lowg.at[k], lowg.at[k], lg_s.at[j], lg_r.at[k], {"rep": j}))
    for m in from_rep:
        for j in [f] + from_fs:
            arrived(half.at[m, j], hr_s.at[j, m], hr_r.at[j, m], {"rep": m})
        weights(m, scale)
    def block_of(i, j, m):
        copy, rows, width, _ = outs[i]
        return copy.at[cols(j, rows), cols(m, width)]

    def relay(j):
        for i, source, to in ((0, near, far), (1, far, near)):
            block = block_of(i, j, source)
            arrived(block, cr_s.at[i, j, source], cr_r.at[i, j, source], {"rep": source})
            sent.append(send(block, block, cr_s.at[i, j, beyond], cr_r.at[i, j, source], {"rep": to}))

    for step, j in enumerate(from_fs):
        for i in range(2):
            block = block_of(i, j, k)
            arrived(block, cz_s.at[i, j], cz_r.at[i, j], {"fs": j})
            for m in targets:
                sent.append(send(block, block, cr_s.at[i, j, m], cr_r.at[i, j, k], {"rep": m}))
        if across and step:
            relay(from_fs[step - 1])
    if across and from_fs:
        relay(from_fs[-1])
    for m in [k] + rep_peers:
        if m is not k:
            arrived(lowg.at[m], lg_s.at[m], lg_r.at[m], {"rep": m})
        block = lowg[m]
        at_q, at_o = cols(m, quarter_q), cols(m, quarter_o)
        nfq[:, at_q], nsq[:, at_q], _ = update(block[:, :quarter_q], fq_ref[:, at_q], sq_ref[:, at_q])
        nfo[:, at_o], nso[:, at_o], _ = update(block[:, quarter_q:], fo_ref[:, at_o], so_ref[:, at_o])
    late = ((1, near), (0, far), (0, beyond), (1, beyond)) if across else [(i, m) for m in from_rep for i in range(2)]
    for j in from_fs:
        for i, m in late:
            arrived(block_of(i, j, m), cr_s.at[i, j, m], cr_r.at[i, j, m], {"rep": m})
    for copy in sent:
        copy.wait_send()


def place(*refs):
    count = len(refs) // 2
    sems = refs[-1]
    copies = [pltpu.make_async_copy(refs[i], refs[count + i], sems.at[i]) for i in range(count)]
    for copy in copies:
        copy.start()
    for copy in copies:
        copy.wait()


def solution(mesh):
    n, r, tp = mesh.shape["fs"], mesh.shape["rep"], mesh.shape["tp"]

    def local(*args):
        x, qc, a, oc, pq, po, wq, wo, fq, sq, fo, so = args
        rank = pq.shape[1]
        low_rows = fq.shape[0]
        wide = (fq.shape[1] + fo.shape[1]) // r
        entries = rank * (fq.shape[1] + fo.shape[1]) * tp
        shape = jax.ShapeDtypeStruct
        like = lambda v: shape(v.shape, v.dtype)
        dma = pltpu.SemaphoreType.DMA
        made = pl.pallas_call(
            functools.partial(kernel, n, r, tp, entries),
            out_shape=(
                like(wq), like(wo), like(wq), like(wo), like(fq), like(sq), like(fo), like(so),
                shape((n * wq.shape[0], wq.shape[1]), BF16),
                shape((n * wo.shape[0], wo.shape[1]), BF16),
            ),
            in_specs=[pl.BlockSpec(memory_space=pltpu.VMEM)] * 12,
            out_specs=[pl.BlockSpec(memory_space=pltpu.VMEM)] * 10,
            scratch_shapes=[
                pltpu.VMEM((n,) + pq.shape, BF16),
                pltpu.VMEM((n,) + po.shape, BF16),
                pltpu.VMEM((r,) + x.shape, BF16),
                pltpu.VMEM((r,) + a.shape, BF16),
                pltpu.VMEM((r, qc.shape[0], qc.shape[1] // r), BF16),
                pltpu.VMEM((r, oc.shape[0], oc.shape[1] // r), BF16),
                pltpu.VMEM((n, low_rows, wide), F32),
                pltpu.VMEM((n, low_rows, wide), F32),
                pltpu.VMEM((r, low_rows, wide), F32),
                pltpu.VMEM((r, n, low_rows, wide), BF16),
                pltpu.VMEM((n, 8, 128), F32),
                pltpu.VMEM((r, 8, 128), F32),
                pltpu.VMEM((tp, 8, 128), F32),
                dma((2, n)), dma((2, n)), dma((2, n)), dma((2, n)),
                dma((4, r)), dma((4, r)), dma((4, r)), dma((4, r)), dma((2, r)), dma((2, r)), dma((n,)), dma((n,)), dma((r,)), dma((r,)),
                dma((n,)), dma((n,)), dma((n, r)), dma((n, r)),
                dma((n,)), dma((n,)), dma((r,)), dma((r,)), dma((1,)), dma((1,)),
                dma((2, n)), dma((2, n)), dma((2, n, r)), dma((2, n, r)),
            ],
            compiler_params=pltpu.CompilerParams(collective_id=0, has_side_effects=True),
        )(*args)
        return pl.pallas_call(
            place,
            out_shape=tuple(like(v) for v in made),
            in_specs=[pl.BlockSpec(memory_space=pltpu.VMEM)] * len(made),
            out_specs=[pl.BlockSpec(memory_space=pl.ANY)] * len(made),
            scratch_shapes=[dma((len(made),))],
        )(*made)

    both, rows = P(("fs", "rep"), "tp"), P("fs", "tp")
    whole = P(("fs", "rep"), None)
    return jax.shard_map(
        local,
        mesh=mesh,
        in_specs=(whole, both, whole, both, P("fs", None), P("fs", None)) + (rows,) * 6,
        out_specs=(rows,) * 8 + (P(None, "tp"),) * 2,
        check_vma=False,
    )
```
